32 devices in a mesh: sp: 16 (over z, y, core), tp: 2 (over x).
Axes of the slice: x: 2, y: 2, z: 4, core: 2. Of those that a mesh axis runs over, the one named last changes fastest.
Arguments:
- tokens: bfloat16 [4096, 2048], P('sp'), may hold values from -28 to 28
- query_weight: bfloat16 [2048, 1536], P(None, 'tp'), may hold values from -0.125 to 0.125
- key_weight: bfloat16 [2048, 1536], P(None, 'tp'), may hold values from -0.125 to 0.125
- value_weight: bfloat16 [2048, 1536], P(None, 'tp'), may hold values from -0.125 to 0.125
- out_weight: bfloat16 [512, 2048], P(None, 'tp'), may hold values from -1 to 1
Outputs:
- mixed: bfloat16 [4096, 2048], P('sp', 'tp')
- total_log: float32 [4, 4096], P('tp', 'sp')
The draws below stay inside these ranges and needn't reach their ends.
All inputs are finite; a program needn't handle non-finite values.
Results may differ from the reference program's by a relative error of at most 0.012.
The reference program's roundings to bfloat16 on the way (of `queries`, `probs` and `merged`) count: a program that leaves them out, or rounds other values in their place, can miss the bound.
Values may be sent and summed in bfloat16 or wider, within the bound.
A program may use at most 64 MiB of HBM per device.

```python
import jax
import jax.numpy as jnp
from jax import lax

D = 2048
HEADS = 4
HEAD_DIM = 128
NEAR_WINDOW = 128
MIDDLE_WINDOW = 512
MIDDLE_DILATION = 4
FAR_WINDOW = 2048
FAR_DILATION = 16
TOK_DEV = 256
TOKENS = 4096
N_SP = 16


def draw_tokens(key, part):
    first_key, second_key, third_key = jax.random.split(key, 3)
    return jnp.clip(jax.random.normal(first_key, (TOKENS, D), jnp.float32), -6.0, 6.0).astype(jnp.bfloat16)


def block_scale(key, extent, cuts, low, largest):
    loudness = 1.0
    for axis_at, shards_of in cuts:
        steps = jax.random.uniform(jax.random.fold_in(jax.random.fold_in(key, 6), axis_at), (shards_of,), jnp.float32, low / len(cuts), largest / len(cuts))
        loudness = loudness * jnp.repeat(jnp.exp(steps), extent[axis_at] // shards_of).reshape((-1,) + (1,) * (len(extent) - 1 - axis_at))
    return loudness


def gaussian(own_key, dims, deviation, limit, cuts=(), kind=jnp.bfloat16):
    level = block_scale(own_key, dims, cuts, -0.22, 0.18) if cuts else 1.0
    array = jax.random.normal(own_key, dims, jnp.float32) * deviation * level
    return jnp.minimum(jnp.maximum(array, -limit), limit).astype(kind)


def setup_inputs(seed: int = 0) -> dict:
    splits = jax.random.split(jax.random.key(seed), 6)
    tokens = draw_tokens(jax.random.fold_in(splits[5], 71), 0)
    query_weight = gaussian(splits[1], (D, HEADS * 3 * HEAD_DIM), D ** -0.5, 0.125, ((1, 2),))
    key_weight = gaussian(splits[2], (D, HEADS * 3 * HEAD_DIM), D ** -0.5, 0.125, ((1, 2),))
    value_weight = gaussian(splits[3], (D, HEADS * 3 * HEAD_DIM), D ** -0.5, 0.125, ((1, 2),))
    out_weight = gaussian(splits[4], (HEADS * HEAD_DIM, D), (HEADS * HEAD_DIM // 16) ** -0.5, 1.0, ((1, 2),))
    return dict(tokens=tokens, query_weight=query_weight, key_weight=key_weight, value_weight=value_weight, out_weight=out_weight)


def window_table():
    return ((NEAR_WINDOW, 1), (MIDDLE_WINDOW, MIDDLE_DILATION), (FAR_WINDOW, FAR_DILATION))


def attend_group(group_queries, buffer, window, dilation, first_key, slopes_here):
    row_count = group_queries.shape[0]
    head_count = group_queries.shape[1]
    head_size = group_queries.shape[2]
    query_split = group_queries.reshape(row_count // dilation, dilation, head_count, head_size)
    key_split = buffer[0].reshape(-1, dilation, head_count, head_size)
    value_split = buffer[1].reshape(-1, dilation, head_count, head_size)
    scores = jnp.einsum("mrhe,nrhe->rhmn", query_split.astype(jnp.float32), key_split.astype(jnp.float32)) * head_size ** -0.5
    grid_shape = (row_count // dilation, key_split.shape[0])
    query_slot = lax.broadcasted_iota(jnp.int32, grid_shape, 0)
    key_slot = lax.broadcasted_iota(jnp.int32, grid_shape, 1)
    spacing = query_slot + window // dilation - key_slot
    residue = lax.broadcasted_iota(jnp.int32, (dilation, 1, 1), 0)
    key_place = first_key + residue + dilation * key_slot[None]
    valid = (spacing[None] >= 0) & (spacing[None] <= window // dilation) & (key_place >= 0)
    scores = scores - slopes_here[None, :, None, None] * (dilation * spacing).astype(scores.dtype)[None, None]
    masked = jnp.where(valid[:, None], scores, -jnp.inf)
    highest = jnp.max(masked, axis=-1, keepdims=True)
    log_sum = highest + jnp.log(jnp.sum(jnp.exp(masked - highest), axis=-1, keepdims=True))
    probs = jnp.exp(masked - log_sum).astype(jnp.bfloat16)
    attended = jnp.einsum("rhmn,nrhe->mrhe", probs.astype(jnp.float32), value_split.astype(jnp.float32))
    attended = attended.reshape(row_count, head_count, head_size)
    log_rows = jnp.transpose(log_sum[..., 0], (1, 2, 0)).reshape(head_count, row_count)
    return attended, log_rows


def reference(tokens, query_weight, key_weight, value_weight, out_weight):
    def project(weight_matrix):
        product = jnp.dot(tokens, weight_matrix, preferred_element_type=jnp.float32)
        return product.astype(jnp.bfloat16).reshape(TOKENS, HEADS, 3, HEAD_DIM)

    queries = project(query_weight)
    keys_all = project(key_weight)
    values_all = project(value_weight)
    stacked = jnp.stack((keys_all, values_all))
    padding = jnp.zeros((2, FAR_WINDOW, HEADS, 3, HEAD_DIM), stacked.dtype)
    padded = jnp.concatenate((padding, stacked), axis=1)
    head_ids = jnp.arange(HEADS).astype(jnp.float32)

    def block_step(block_index):
        first_row = block_index * TOK_DEV
        query_block = lax.dynamic_slice_in_dim(queries, first_row, TOK_DEV, 0)
        outputs = []
        logs = []
        for group_index, (window, dilation) in enumerate(window_table()):
            begin = (first_row + FAR_WINDOW - window).astype(jnp.int32)
            buffer = lax.dynamic_slice_in_dim(padded, begin, window + TOK_DEV, 1)[:, :, :, group_index]
            slopes_here = 2.0 ** (3.0 - 8.0 * (head_ids + 1.0) / HEADS) / window
            attended, log_rows = attend_group(query_block[:, :, group_index], buffer, window, dilation, first_row - window, slopes_here)
            outputs.append(attended)
            logs.append(log_rows)
        stacked_logs = jnp.stack(logs)
        highest = jnp.max(stacked_logs, axis=0)
        total_block = highest + jnp.log(jnp.sum(jnp.exp(stacked_logs - highest), axis=0))
        mixing = jnp.exp(stacked_logs - total_block)
        merged_block = outputs[0] * jnp.transpose(mixing[0])[:, :, None]
        merged_block = merged_block + outputs[1] * jnp.transpose(mixing[1])[:, :, None]
        merged_block = merged_block + outputs[2] * jnp.transpose(mixing[2])[:, :, None]
        return merged_block.astype(jnp.bfloat16), total_block

    merged_blocks, totals = lax.map(block_step, jnp.arange(N_SP, dtype=jnp.int32))
    merged = merged_blocks.reshape(TOKENS, HEADS * HEAD_DIM)
    mixed = jnp.dot(merged, out_weight, preferred_element_type=jnp.float32).astype(jnp.bfloat16)
    total_log = jnp.transpose(totals, (1, 0, 2)).reshape(HEADS, TOKENS)
    return mixed, total_log
```

```python
import functools
import jax
import jax.numpy as jnp
from jax import lax
from jax.experimental import pallas as pl
from jax.experimental.pallas import tpu as pltpu
from jax.sharding import PartitionSpec as P

HEADS = 4
HEAD_DIM = 128
NEAR_WINDOW = 128
MIDDLE_WINDOW = 512
MIDDLE_DILATION = 4
FAR_WINDOW = 2048
FAR_DILATION = 16


def from_behind(block, axis, distance):
    devices = range(lax.axis_size(axis))
    route = [(i - distance, i) for i in devices if i - distance in devices]
    return lax.ppermute(block, axis, route)


def window_table():
    return ((NEAR_WINDOW, 1), (MIDDLE_WINDOW, MIDDLE_DILATION), (FAR_WINDOW, FAR_DILATION))


def tail_counts(row_count, distance, held_rows):
    counts = []
    for entry, available in zip(window_table(), held_rows):
        counts.append(max(0, min(available, entry[0] - (distance - 1) * row_count)))
    return counts


def pack_tails(sources, counts):
    selected = [
        source[:, source.shape[1] - amount :]
        for source, amount in zip(sources, counts)
        if amount > 0
    ]
    return jnp.concatenate(selected, axis=1)


def unpack_rows(packed, counts):
    result = []
    cursor = 0
    for amount in counts:
        result.append(packed[:, cursor : cursor + amount])
        cursor = cursor + amount
    return result


def attend_group(group_queries, buffer, window, dilation, first_key, slopes_here):
    row_count = group_queries.shape[0]
    head_count = group_queries.shape[1]
    head_size = group_queries.shape[2]
    query_split = group_queries.reshape(row_count // dilation, dilation, head_count, head_size)
    key_split = buffer[0].reshape(-1, dilation, head_count, head_size)
    value_split = buffer[1].reshape(-1, dilation, head_count, head_size)
    scores = jnp.einsum(
        "mrhe,nrhe->rhmn", query_split, key_split, preferred_element_type=jnp.float32
    ) * head_size ** (-0.5)
    grid_shape = (row_count // dilation, key_split.shape[0])
    query_slot = lax.broadcasted_iota(jnp.int32, grid_shape, 0)
    key_slot = lax.broadcasted_iota(jnp.int32, grid_shape, 1)
    spacing = query_slot + window // dilation - key_slot
    residue = lax.broadcasted_iota(jnp.int32, (dilation, 1, 1), 0)
    key_place = first_key + residue + dilation * key_slot[None]
    valid = (spacing[None] >= 0) & (spacing[None] <= window // dilation) & (key_place >= 0)
    scores = (
        scores
        - slopes_here[None, :, None, None] * (dilation * spacing).astype(jnp.float32)[None, None]
    )
    masked = jnp.where(valid[:, None], scores, -jnp.inf)
    highest = jnp.max(masked, axis=-1, keepdims=True)
    log_sum = highest + jnp.log(jnp.sum(jnp.exp(masked - highest), axis=-1, keepdims=True))
    probs = jnp.exp(masked - log_sum).astype(jnp.bfloat16)
    attended = jnp.einsum("rhmn,nrhe->mrhe", probs, value_split, preferred_element_type=jnp.float32)
    attended = attended.reshape(row_count, head_count, head_size)
    log_rows = jnp.transpose(log_sum[..., 0], (1, 2, 0)).reshape(head_count, row_count)
    return (attended, log_rows)


def local(tokens, query_weight, key_weight, value_weight, out_weight):
    rows_here = tokens.shape[0]
    local_heads = query_weight.shape[1] // (3 * HEAD_DIM)

    def project(weight_matrix):
        product = jnp.dot(tokens, weight_matrix, preferred_element_type=jnp.float32)
        return product.astype(jnp.bfloat16).reshape(rows_here, local_heads, 3, HEAD_DIM)

    queries = project(query_weight)
    keys_all = project(key_weight)
    values_all = project(value_weight)
    table = window_table()
    own = [jnp.stack((keys_all[:, :, index], values_all[:, :, index])) for index in range(3)]
    held = list(own)
    span_now = 1
    while span_now * rows_here < FAR_WINDOW + rows_here:
        counts = tail_counts(rows_here, span_now, [item.shape[1] for item in held])
        packed = pack_tails(held, counts)
        arrived = from_behind(packed, "sp", span_now)
        pieces_in = unpack_rows(arrived, counts)
        for index in range(3):
            if counts[index] > 0:
                joined = jnp.concatenate((pieces_in[index], held[index]), axis=1)
                held[index] = joined
        span_now = span_now * 2
    priors = [held[index][:, : table[index][0]] for index in range(3)]
    position_start = lax.axis_index("sp") * rows_here
    head_ids = (
        lax.axis_index("tp") * local_heads + jnp.arange(local_heads, dtype=jnp.int32)
    ).astype(jnp.float32)
    outputs = []
    logs = []
    for index, (window, dilation) in enumerate(table):
        buffer = jnp.concatenate((priors[index], own[index]), axis=1)
        slopes_here = 2.0 ** (3.0 - 8.0 * (head_ids + 1.0) / HEADS) / window
        attended, log_rows = attend_group(
            queries[:, :, index], buffer, window, dilation, position_start - window, slopes_here
        )
        outputs.append(attended)
        logs.append(log_rows)
    stacked_logs = jnp.stack(logs)
    highest = jnp.max(stacked_logs, axis=0)
    total_log = highest + jnp.log(jnp.sum(jnp.exp(stacked_logs - highest), axis=0))
    mixing = jnp.exp(stacked_logs - total_log)
    merged = outputs[0] * jnp.transpose(mixing[0])[:, :, None]
    merged = merged + outputs[1] * jnp.transpose(mixing[1])[:, :, None]
    merged = merged + outputs[2] * jnp.transpose(mixing[2])[:, :, None]
    merged = merged.astype(jnp.bfloat16).reshape(rows_here, local_heads * HEAD_DIM)
    mixed = jnp.dot(
        lax.all_gather(merged, "tp", axis=1, tiled=True),
        out_weight,
        preferred_element_type=jnp.float32,
    ).astype(jnp.bfloat16)
    return (mixed, total_log)


MESH = pl.DeviceIdType.MESH
MASKED = -1e30


def attend(query, key, value, slope, distance, valid):
    scores = lax.dot_general(
        query, key, (((1,), (1,)), ((), ())), preferred_element_type=jnp.float32
    ) * HEAD_DIM ** (-0.5)
    scores = jnp.where(valid, scores - slope * distance, MASKED)
    highest = jnp.max(scores, axis=-1, keepdims=True)
    weights = jnp.exp(scores - highest)
    total = jnp.sum(weights, axis=-1, keepdims=True)
    probs = (weights * (1.0 / total)).astype(jnp.bfloat16)
    attended = jnp.dot(probs, value, preferred_element_type=jnp.float32)
    return attended, highest + jnp.log(total)


def swap_matrix(rows, width):
    shift = width.bit_length() - 1
    row = lax.broadcasted_iota(jnp.int32, (rows, rows), 0)
    column = lax.broadcasted_iota(jnp.int32, (rows, rows), 1)
    source = ((row & (width - 1)) << shift) + (row >> shift)
    return jnp.where(column == source, 1.0, 0.0).astype(jnp.bfloat16)


def kernel(
    n, n_tp, local_heads,
    tok_hbm, wq_hbm, wk_hbm, wv_hbm, wo_hbm,
    mixed_ref, log_ref,
    tok, weight, wo, far_send, far_held, back_send, back_held,
    mid_query, mid_own, mid_held, near_query, near_own, near_held,
    merged_own, merged_held,
    load_sem, far_ssem, far_rsem, back_ssem, back_rsem,
    mid_ssem, mid_rsem, near_ssem, near_rsem, merged_ssem, merged_rsem,
):
    me = lax.axis_index("sp")
    tp = lax.axis_index("tp")
    rows = tok.shape[0]
    width = local_heads * HEAD_DIM
    chunk = rows // n
    peer = 1 - tp

    loads = {}
    tok_load = pltpu.make_async_copy(tok_hbm, tok, load_sem.at[0])
    tok_load.start()
    count = 1
    for group in (2, 1, 0):
        loads[group] = []
        for part, source in enumerate((wq_hbm, wk_hbm, wv_hbm)):
            for head in range(local_heads):
                copy = pltpu.make_async_copy(
                    source.at[:, pl.ds((head * 3 + group) * HEAD_DIM, HEAD_DIM)],
                    weight.at[group, :, pl.ds((part * local_heads + head) * HEAD_DIM, HEAD_DIM)],
                    load_sem.at[count],
                )
                copy.start()
                loads[group].append(copy)
                count += 1
    wo_load = pltpu.make_async_copy(wo_hbm, wo, load_sem.at[count])
    wo_load.start()

    barrier = pltpu.get_barrier_semaphore()

    def greet(k, carry):
        pl.semaphore_signal(barrier, inc=1, device_id=(lax.rem(me + k, n), tp), device_id_type=MESH)
        return carry

    lax.fori_loop(1, n, greet, 0)
    pl.semaphore_signal(barrier, inc=1, device_id=(me, peer), device_id_type=MESH)

    @pl.when(me < 2)
    def _():
        mid_held[0] = jnp.zeros((rows, 2 * width), jnp.bfloat16)

    @pl.when(me < 1)
    def _():
        mid_held[1] = jnp.zeros((rows, 2 * width), jnp.bfloat16)
        near_held[...] = jnp.zeros((NEAR_WINDOW, 2 * width), jnp.bfloat16)

    def project(group, first, extent):
        return jnp.dot(
            tok[...], weight[group, :, first : first + extent], preferred_element_type=jnp.float32
        ).astype(jnp.bfloat16)

    def at_rows(index):
        return pl.ds(pl.multiple_of(index * chunk, chunk), chunk)

    swap = swap_matrix(rows, n)
    tok_load.wait()
    for copy in loads[2]:
        copy.wait()
    for part in range(3):
        block = project(2, part * width, width)
        far_send[:, part * width : (part + 1) * width] = jnp.dot(
            swap, block, preferred_element_type=jnp.float32
        ).astype(jnp.bfloat16)
    far_held[at_rows(me), :] = far_send[at_rows(me), :]

    def exchange(source, target, ssem, rsem, k, outgoing):
        to = lax.rem(me + k, n)
        come = lax.rem(me + n - k, n)
        return pltpu.make_async_remote_copy(
            src_ref=source.at[at_rows(to)],
            dst_ref=target.at[at_rows(me if outgoing else come)],
            send_sem=ssem.at[k],
            recv_sem=rsem.at[k],
            device_id=(to, tp),
            device_id_type=MESH,
        )

    def far_copy(k, outgoing):
        return exchange(far_send, far_held, far_ssem, far_rsem, k, outgoing)

    def back_copy(k, outgoing):
        return exchange(back_send, back_held, back_ssem, back_rsem, k, outgoing)

    def each(action):
        def step(k, carry):
            action(k)
            return carry

        lax.fori_loop(1, n, step, 0)

    pl.semaphore_wait(barrier, n)
    each(lambda k: far_copy(k, True).start())

    for copy in loads[1]:
        copy.wait()
    mid_own[:, :width] = project(1, width, width)
    mid_own[:, width:] = project(1, 2 * width, width)

    def mid_copy(slot, hop, source, sem):
        return pltpu.make_async_remote_copy(
            src_ref=source,
            dst_ref=mid_held.at[slot],
            send_sem=mid_ssem.at[sem],
            recv_sem=mid_rsem.at[slot],
            device_id=(lax.rem(me + hop, n), tp),
            device_id_type=MESH,
        )

    def near_copy():
        return pltpu.make_async_remote_copy(
            src_ref=near_own.at[pl.ds(rows - NEAR_WINDOW, NEAR_WINDOW)],
            dst_ref=near_held,
            send_sem=near_ssem,
            recv_sem=near_rsem,
            device_id=(lax.rem(me + 1, n), tp),
            device_id_type=MESH,
        )

    even = lax.rem(me, 2) == 0
    sends_one = me + 1 < n
    sends_two = even & (me + 2 < n)
    relays = even & (me >= 1)

    @pl.when(sends_two)
    def _():
        mid_copy(0, 2, mid_own, 0).start()

    @pl.when(sends_one)
    def _():
        mid_copy(1, 1, mid_own, 1).start()

    for copy in loads[0]:
        copy.wait()
    near_own[:, :width] = project(0, width, width)
    near_own[:, width:] = project(0, 2 * width, width)

    @pl.when(sends_one)
    def _():
        near_copy().start()

    mid_query[...] = project(1, 0, width)
    near_query[...] = project(0, 0, width)

    def slope_of(head, window):
        number = tp * local_heads + head
        slope = jnp.float32(0.0)
        for index in range(HEADS):
            value = 2.0 ** (3.0 - 8.0 * (index + 1.0) / HEADS) / window
            slope = jnp.where(number == index, jnp.float32(value), slope)
        return slope

    def spacing(row_count, key_count, offset):
        row = lax.broadcasted_iota(jnp.int32, (row_count, key_count), 0)
        column = lax.broadcasted_iota(jnp.int32, (row_count, key_count), 1)
        return row + offset - column, column

    each(lambda k: far_copy(k, False).wait_recv())
    reach = FAR_WINDOW // FAR_DILATION
    apart, column = spacing(rows, rows, 0)
    valid = (apart >= 0) & (apart <= reach)
    distance = (apart * FAR_DILATION).astype(jnp.float32)
    lane = lax.broadcasted_iota(jnp.int32, (rows, HEAD_DIM), 1)
    packed = jnp.zeros((rows, HEAD_DIM), jnp.float32)
    for head in range(local_heads):
        at = head * HEAD_DIM
        attended, log_sum = attend(
            far_held[:, at : at + HEAD_DIM],
            far_held[:, width + at : width + at + HEAD_DIM],
            far_held[:, 2 * width + at : 2 * width + at + HEAD_DIM],
            slope_of(head, FAR_WINDOW), distance, valid,
        )
        back_send[:, at : at + HEAD_DIM] = attended.astype(jnp.bfloat16)
        rest = log_sum
        for term in range(3):
            piece = rest.astype(jnp.bfloat16).astype(jnp.float32)
            packed = jnp.where(lane == 3 * head + term, piece, packed)
            rest = rest - piece
    back_send[:, width:] = packed.astype(jnp.bfloat16)
    back_held[at_rows(me), :] = back_send[at_rows(me), :]
    each(lambda k: back_copy(k, True).start())

    @pl.when(me >= 1)
    def _():
        near_copy().wait_recv()
        mid_copy(1, 1, mid_own, 1).wait_recv()

    @pl.when(relays)
    def _():
        mid_copy(0, 1, mid_held.at[1], 0 + 2).start()

    apart, column = spacing(rows, NEAR_WINDOW + rows, NEAR_WINDOW)
    valid = (apart >= 0) & (apart <= NEAR_WINDOW) & (column + me * rows >= NEAR_WINDOW)
    distance = apart.astype(jnp.float32)
    near = []
    for head in range(local_heads):
        at = head * HEAD_DIM
        key = jnp.concatenate((near_held[:, at : at + HEAD_DIM], near_own[:, at : at + HEAD_DIM]), axis=0)
        at2 = width + at
        value = jnp.concatenate((near_held[:, at2 : at2 + HEAD_DIM], near_own[:, at2 : at2 + HEAD_DIM]), axis=0)
        near.append(attend(near_query[:, at : at + HEAD_DIM], key, value, slope_of(head, NEAR_WINDOW), distance, valid))

    @pl.when(me >= 2)
    def _():
        mid_copy(0, 2, mid_own, 0).wait_recv()

    apart, column = spacing(rows, MIDDLE_WINDOW + rows, MIDDLE_WINDOW)
    valid = (apart >= 0) & (apart <= MIDDLE_WINDOW) & ((apart & (MIDDLE_DILATION - 1)) == 0)
    valid = valid & (column + me * rows >= MIDDLE_WINDOW)
    distance = apart.astype(jnp.float32)
    middle = []
    for head in range(local_heads):
        at = head * HEAD_DIM
        key = jnp.concatenate([x[:, at : at + HEAD_DIM] for x in (mid_held[0], mid_held[1], mid_own[...])], axis=0)
        at2 = width + at
        value = jnp.concatenate([x[:, at2 : at2 + HEAD_DIM] for x in (mid_held[0], mid_held[1], mid_own[...])], axis=0)
        middle.append(attend(mid_query[:, at : at + HEAD_DIM], key, value, slope_of(head, MIDDLE_WINDOW), distance, valid))

    each(lambda k: back_copy(k, False).wait_recv())
    far = jnp.dot(swap, back_held[...], preferred_element_type=jnp.float32)
    parts = far[:, width:]
    totals = jnp.zeros((rows, HEAD_DIM), jnp.float32)
    for head in range(local_heads):
        at = head * HEAD_DIM
        far_log = jnp.sum(
            jnp.where((lane >= 3 * head) & (lane < 3 * head + 3), parts, 0.0), axis=-1, keepdims=True
        )
        near_log, middle_log = near[head][1], middle[head][1]
        highest = jnp.maximum(jnp.maximum(near_log, middle_log), far_log)
        total = highest + jnp.log(
            jnp.exp(near_log - highest) + jnp.exp(middle_log - highest) + jnp.exp(far_log - highest)
        )
        merged = near[head][0] * jnp.exp(near_log - total)
        merged = merged + middle[head][0] * jnp.exp(middle_log - total)
        merged = merged + far[:, at : at + HEAD_DIM] * jnp.exp(far_log - total)
        merged_own[:, at : at + HEAD_DIM] = merged.astype(jnp.bfloat16)
        totals = jnp.where(lane == head, total, totals)

    swap_merged = pltpu.make_async_remote_copy(
        src_ref=merged_own,
        dst_ref=merged_held,
        send_sem=merged_ssem,
        recv_sem=merged_rsem,
        device_id=(me, peer),
        device_id_type=MESH,
    )
    swap_merged.start()
    log_ref[...] = jnp.transpose(totals)[:local_heads]
    wo_load.wait()
    half = mixed_ref.shape[1] // 4

    def wo_rows(index):
        return pl.ds(pl.multiple_of(index * width, width), width)

    own_terms = [
        jnp.dot(merged_own[...], wo[wo_rows(tp), c * half : (c + 1) * half], preferred_element_type=jnp.float32)
        for c in range(4)
    ]
    swap_merged.wait_recv()
    for c in range(4):
        other = jnp.dot(
            merged_held[...], wo[wo_rows(peer), c * half : (c + 1) * half], preferred_element_type=jnp.float32
        )
        mixed_ref[:, c * half : (c + 1) * half] = (own_terms[c] + other).astype(jnp.bfloat16)

    swap_merged.wait_send()
    each(lambda k: far_copy(k, True).wait_send())
    each(lambda k: back_copy(k, True).wait_send())

    @pl.when(sends_two)
    def _():
        mid_copy(0, 2, mid_own, 0).wait_send()

    @pl.when(sends_one)
    def _():
        mid_copy(1, 1, mid_own, 1).wait_send()
        near_copy().wait_send()

    @pl.when(relays)
    def _():
        mid_copy(0, 1, mid_held.at[1], 2).wait_send()


def fused(n, n_tp, tokens, query_weight, key_weight, value_weight, out_weight):
    rows, depth = tokens.shape
    columns = query_weight.shape[1]
    local_heads = columns // (3 * HEAD_DIM)
    width = local_heads * HEAD_DIM
    dma = pltpu.SemaphoreType.DMA
    half = jnp.bfloat16
    return pl.pallas_call(
        functools.partial(kernel, n, n_tp, local_heads),
        out_shape=(
            jax.ShapeDtypeStruct((rows, out_weight.shape[1]), half),
            jax.ShapeDtypeStruct((local_heads, rows), jnp.float32),
        ),
        in_specs=[pl.BlockSpec(memory_space=pl.ANY)] * 5,
        out_specs=(pl.BlockSpec(memory_space=pltpu.VMEM), pl.BlockSpec(memory_space=pltpu.VMEM)),
        scratch_shapes=[
            pltpu.VMEM((rows, depth), half),
            pltpu.VMEM((3, depth, columns), half),
            pltpu.VMEM(out_weight.shape, half),
            pltpu.VMEM((rows, columns), half),
            pltpu.VMEM((rows, columns), half),
            pltpu.VMEM((rows, width + HEAD_DIM), half),
            pltpu.VMEM((rows, width + HEAD_DIM), half),
            pltpu.VMEM((rows, width), half),
            pltpu.VMEM((rows, 2 * width), half),
            pltpu.VMEM((2, rows, 2 * width), half),
            pltpu.VMEM((rows, width), half),
            pltpu.VMEM((rows, 2 * width), half),
            pltpu.VMEM((NEAR_WINDOW, 2 * width), half),
            pltpu.VMEM((rows, width), half),
            pltpu.VMEM((rows, width), half),
            dma((2 + 9 * local_heads,)),
            dma((n,)), dma((n,)), dma((n,)), dma((n,)),
            dma((3,)), dma((2,)), dma(()), dma(()), dma(()), dma(()),
        ],
        compiler_params=pltpu.CompilerParams(
            collective_id=0, has_side_effects=True, vmem_limit_bytes=60000 * 1024
        ),
    )(tokens, query_weight, key_weight, value_weight, out_weight)


def solution(mesh):
    n, n_tp = mesh.shape["sp"], mesh.shape["tp"]
    if n == FAR_DILATION and n_tp == 2:
        body = functools.partial(fused, n, n_tp)
    else:
        body = local
    return jax.shard_map(
        body,
        mesh=mesh,
        in_specs=(P("sp", None), P(None, "tp"), P(None, "tp"), P(None, "tp"), P(None, "tp")),
        out_specs=(P("sp", "tp"), P("tp", "sp")),
        check_vma=False,
    )
```

```python
import functools
import jax
import jax.numpy as jnp
from jax import lax
from jax.experimental import pallas as pl
from jax.experimental.pallas import tpu as pltpu
from jax.sharding import PartitionSpec as P

HEADS = 4
HEAD_DIM = 128
NEAR_WINDOW = 128
MIDDLE_WINDOW = 512
MIDDLE_DILATION = 4
FAR_WINDOW = 2048
FAR_DILATION = 16


def from_behind(block, axis, distance):
    devices = range(lax.axis_size(axis))
    route = [(i - distance, i) for i in devices if i - distance in devices]
    return lax.ppermute(block, axis, route)


def window_table():
    return ((NEAR_WINDOW, 1), (MIDDLE_WINDOW, MIDDLE_DILATION), (FAR_WINDOW, FAR_DILATION))


def tail_counts(row_count, distance, held_rows):
    counts = []
    for entry, available in zip(window_table(), held_rows):
        counts.append(max(0, min(available, entry[0] - (distance - 1) * row_count)))
    return counts


def pack_tails(sources, counts):
    selected = [
        source[:, source.shape[1] - amount :]
        for source, amount in zip(sources, counts)
        if amount > 0
    ]
    return jnp.concatenate(selected, axis=1)


def unpack_rows(packed, counts):
    result = []
    cursor = 0
    for amount in counts:
        result.append(packed[:, cursor : cursor + amount])
        cursor = cursor + amount
    return result


def attend_group(group_queries, buffer, window, dilation, first_key, slopes_here):
    row_count = group_queries.shape[0]
    head_count = group_queries.shape[1]
    head_size = group_queries.shape[2]
    query_split = group_queries.reshape(row_count // dilation, dilation, head_count, head_size)
    key_split = buffer[0].reshape(-1, dilation, head_count, head_size)
    value_split = buffer[1].reshape(-1, dilation, head_count, head_size)
    scores = jnp.einsum(
        "mrhe,nrhe->rhmn", query_split, key_split, preferred_element_type=jnp.float32
    ) * head_size ** (-0.5)
    grid_shape = (row_count // dilation, key_split.shape[0])
    query_slot = lax.broadcasted_iota(jnp.int32, grid_shape, 0)
    key_slot = lax.broadcasted_iota(jnp.int32, grid_shape, 1)
    spacing = query_slot + window // dilation - key_slot
    residue = lax.broadcasted_iota(jnp.int32, (dilation, 1, 1), 0)
    key_place = first_key + residue + dilation * key_slot[None]
    valid = (spacing[None] >= 0) & (spacing[None] <= window // dilation) & (key_place >= 0)
    scores = (
        scores
        - slopes_here[None, :, None, None] * (dilation * spacing).astype(jnp.float32)[None, None]
    )
    masked = jnp.where(valid[:, None], scores, -jnp.inf)
    highest = jnp.max(masked, axis=-1, keepdims=True)
    log_sum = highest + jnp.log(jnp.sum(jnp.exp(masked - highest), axis=-1, keepdims=True))
    probs = jnp.exp(masked - log_sum).astype(jnp.bfloat16)
    attended = jnp.einsum("rhmn,nrhe->mrhe", probs, value_split, preferred_element_type=jnp.float32)
    attended = attended.reshape(row_count, head_count, head_size)
    log_rows = jnp.transpose(log_sum[..., 0], (1, 2, 0)).reshape(head_count, row_count)
    return (attended, log_rows)


def local(tokens, query_weight, key_weight, value_weight, out_weight):
    rows_here = tokens.shape[0]
    local_heads = query_weight.shape[1] // (3 * HEAD_DIM)

    def project(weight_matrix):
        product = jnp.dot(tokens, weight_matrix, preferred_element_type=jnp.float32)
        return product.astype(jnp.bfloat16).reshape(rows_here, local_heads, 3, HEAD_DIM)

    queries = project(query_weight)
    keys_all = project(key_weight)
    values_all = project(value_weight)
    table = window_table()
    own = [jnp.stack((keys_all[:, :, index], values_all[:, :, index])) for index in range(3)]
    held = list(own)
    span_now = 1
    while span_now * rows_here < FAR_WINDOW + rows_here:
        counts = tail_counts(rows_here, span_now, [item.shape[1] for item in held])
        packed = pack_tails(held, counts)
        arrived = from_behind(packed, "sp", span_now)
        pieces_in = unpack_rows(arrived, counts)
        for index in range(3):
            if counts[index] > 0:
                joined = jnp.concatenate((pieces_in[index], held[index]), axis=1)
                held[index] = joined
        span_now = span_now * 2
    priors = [held[index][:, : table[index][0]] for index in range(3)]
    position_start = lax.axis_index("sp") * rows_here
    head_ids = (
        lax.axis_index("tp") * local_heads + jnp.arange(local_heads, dtype=jnp.int32)
    ).astype(jnp.float32)
    outputs = []
    logs = []
    for index, (window, dilation) in enumerate(table):
        buffer = jnp.concatenate((priors[index], own[index]), axis=1)
        slopes_here = 2.0 ** (3.0 - 8.0 * (head_ids + 1.0) / HEADS) / window
        attended, log_rows = attend_group(
            queries[:, :, index], buffer, window, dilation, position_start - window, slopes_here
        )
        outputs.append(attended)
        logs.append(log_rows)
    stacked_logs = jnp.stack(logs)
    highest = jnp.max(stacked_logs, axis=0)
    total_log = highest + jnp.log(jnp.sum(jnp.exp(stacked_logs - highest), axis=0))
    mixing = jnp.exp(stacked_logs - total_log)
    merged = outputs[0] * jnp.transpose(mixing[0])[:, :, None]
    merged = merged + outputs[1] * jnp.transpose(mixing[1])[:, :, None]
    merged = merged + outputs[2] * jnp.transpose(mixing[2])[:, :, None]
    merged = merged.astype(jnp.bfloat16).reshape(rows_here, local_heads * HEAD_DIM)
    mixed = jnp.dot(
        lax.all_gather(merged, "tp", axis=1, tiled=True),
        out_weight,
        preferred_element_type=jnp.float32,
    ).astype(jnp.bfloat16)
    return (mixed, total_log)


MESH = pl.DeviceIdType.MESH
MASKED = -1e30


def attend(query, key, value, slope, distance, valid):
    scores = lax.dot_general(
        query, key, (((1,), (1,)), ((), ())), preferred_element_type=jnp.float32
    ) * HEAD_DIM ** (-0.5)
    scores = jnp.where(valid, scores - slope * distance, MASKED)
    highest = jnp.max(scores, axis=-1, keepdims=True)
    weights = jnp.exp(scores - highest)
    total = jnp.sum(weights, axis=-1, keepdims=True)
    probs = (weights * (1.0 / total)).astype(jnp.bfloat16)
    attended = jnp.dot(probs, value, preferred_element_type=jnp.float32)
    return attended, highest + jnp.log(total)


def swap_matrix(rows, width):
    shift = width.bit_length() - 1
    row = lax.broadcasted_iota(jnp.int32, (rows, rows), 0)
    column = lax.broadcasted_iota(jnp.int32, (rows, rows), 1)
    source = ((row & (width - 1)) << shift) + (row >> shift)
    return jnp.where(column == source, 1.0, 0.0).astype(jnp.bfloat16)


def kernel(
    n, n_tp, local_heads,
    tok_hbm, wq_hbm, wk_hbm, wv_hbm,
    both_ref, totals_ref,
    tok, weight, far_send, far_held, back_send, back_held,
    mid_query, mid_own, mid_held, via_held, near_query, near_own, near_held,
    merged_own, merged_held,
    load_sem, far_ssem, far_rsem, back_ssem, back_rsem,
    mid_ssem, mid_rsem, via_ssem, via_rsem, near_ssem, near_rsem, merged_ssem, merged_rsem,
):
    me = lax.axis_index("sp")
    tp = lax.axis_index("tp")
    rows = tok.shape[0]
    width = local_heads * HEAD_DIM
    chunk = rows // n
    peer = 1 - tp

    loads = {}
    tok_load = pltpu.make_async_copy(tok_hbm, tok, load_sem.at[0])
    tok_load.start()
    count = 1
    for group in (2, 1, 0):
        loads[group] = []
        for part, source in enumerate((wq_hbm, wk_hbm, wv_hbm)):
            for head in range(local_heads):
                copy = pltpu.make_async_copy(
                    source.at[:, pl.ds((head * 3 + group) * HEAD_DIM, HEAD_DIM)],
                    weight.at[group, :, pl.ds((part * local_heads + head) * HEAD_DIM, HEAD_DIM)],
                    load_sem.at[count],
                )
                copy.start()
                loads[group].append(copy)
                count += 1

    barrier = pltpu.get_barrier_semaphore()

    def greet(k, carry):
        pl.semaphore_signal(barrier, inc=1, device_id=(lax.rem(me + k, n), tp), device_id_type=MESH)
        return carry

    lax.fori_loop(1, n, greet, 0)
    pl.semaphore_signal(barrier, inc=1, device_id=(me, peer), device_id_type=MESH)

    @pl.when(me < 2)
    def _():
        mid_held[0] = jnp.zeros((2, rows, width), jnp.bfloat16)

    @pl.when(me < 1)
    def _():
        mid_held[1] = jnp.zeros((2, rows, width), jnp.bfloat16)
        near_held[...] = jnp.zeros((NEAR_WINDOW, 2 * width), jnp.bfloat16)

    def project(group, first, extent):
        return jnp.dot(
            tok[...], weight[group, :, first : first + extent], preferred_element_type=jnp.float32
        ).astype(jnp.bfloat16)

    def at_rows(index):
        return pl.ds(pl.multiple_of(index * chunk, chunk), chunk)

    swap = swap_matrix(rows, n)
    tok_load.wait()
    for copy in loads[2]:
        copy.wait()
    for part in range(3):
        block = project(2, part * width, width)
        far_send[:, part * width : (part + 1) * width] = jnp.dot(
            swap, block, preferred_element_type=jnp.float32
        ).astype(jnp.bfloat16)
    far_held[at_rows(me), :] = far_send[at_rows(me), :]

    def exchange(source, target, ssem, rsem, k, outgoing):
        to = lax.rem(me + k, n)
        come = lax.rem(me + n - k, n)
        return pltpu.make_async_remote_copy(
            src_ref=source.at[at_rows(to)],
            dst_ref=target.at[at_rows(me if outgoing else come)],
            send_sem=ssem.at[k],
            recv_sem=rsem.at[k],
            device_id=(to, tp),
            device_id_type=MESH,
        )

    def far_copy(k, outgoing):
        return exchange(far_send, far_held, far_ssem, far_rsem, k, outgoing)

    def back_copy(k, outgoing):
        return exchange(back_send, back_held, back_ssem, back_rsem, k, outgoing)

    def each(action):
        def step(k, carry):
            action(k)
            return carry

        lax.fori_loop(1, n, step, 0)

    pl.semaphore_wait(barrier, n)
    each(lambda k: far_copy(k, True).start())

    for copy in loads[1]:
        copy.wait()
    mid_own[0] = project(1, width, width)
    mid_own[1] = project(1, 2 * width, width)

    def mid_copy(slot, hop, source, part, sem):
        return pltpu.make_async_remote_copy(
            src_ref=source,
            dst_ref=mid_held.at[slot, part],
            send_sem=mid_ssem.at[sem, part],
            recv_sem=mid_rsem.at[slot, part],
            device_id=(lax.rem(me + hop + n, n), tp),
            device_id_type=MESH,
        )

    def via_copy():
        return pltpu.make_async_remote_copy(
            src_ref=mid_own.at[1],
            dst_ref=via_held,
            send_sem=via_ssem,
            recv_sem=via_rsem,
            device_id=(lax.rem(me + -2 + n, n), tp),
            device_id_type=MESH,
        )

    def near_copy():
        return pltpu.make_async_remote_copy(
            src_ref=near_own.at[pl.ds(rows - NEAR_WINDOW, NEAR_WINDOW)],
            dst_ref=near_held,
            send_sem=near_ssem,
            recv_sem=near_rsem,
            device_id=(lax.rem(me + 1, n), tp),
            device_id_type=MESH,
        )

    even = lax.rem(me, 2) == 0
    sends_one = me + 1 < n
    sends_two = even & (me + 2 < n)
    relays = even & (me >= 1)

    crosses = (lax.rem(me, 4) >= 2) & sends_one & (me + 4 - lax.rem(me, 4) < n)
    forwards = (lax.rem(me, 4) < 2) & (me + 4 - lax.rem(me, 4) < n)
    forward_even = forwards & even
    forward_odd = forwards & jnp.logical_not(even)

    @pl.when(crosses)
    def _():
        via_copy().start()

    @pl.when(sends_two)
    def _():
        mid_copy(0, 2, mid_own.at[0], 0, 0).start()

    @pl.when(sends_one)
    def _():
        mid_copy(1, 1, mid_own.at[0], 0, 1).start()

    @pl.when(sends_two & jnp.logical_not(crosses))
    def _():
        mid_copy(0, 2, mid_own.at[1], 1, 0).start()

    own_value_one = sends_one & jnp.logical_not(crosses & jnp.logical_not(even))

    @pl.when(own_value_one)
    def _():
        mid_copy(1, 1, mid_own.at[1], 1, 1).start()

    for copy in loads[0]:
        copy.wait()
    near_own[:, :width] = project(0, width, width)
    near_own[:, width:] = project(0, 2 * width, width)

    @pl.when(sends_one)
    def _():
        near_copy().start()

    mid_query[...] = project(1, 0, width)
    near_query[...] = project(0, 0, width)

    def slope_of(head, window):
        number = tp * local_heads + head
        slope = jnp.float32(0.0)
        for index in range(HEADS):
            value = 2.0 ** (3.0 - 8.0 * (index + 1.0) / HEADS) / window
            slope = jnp.where(number == index, jnp.float32(value), slope)
        return slope

    def spacing(row_count, key_count, offset):
        row = lax.broadcasted_iota(jnp.int32, (row_count, key_count), 0)
        column = lax.broadcasted_iota(jnp.int32, (row_count, key_count), 1)
        return row + offset - column, column

    each(lambda k: far_copy(k, False).wait_recv())

    @pl.when(forwards)
    def _():
        via_copy().wait_recv()

    @pl.when(forward_even)
    def _():
        mid_copy(0, 4, via_held, 1, 3).start()

    @pl.when(forward_odd)
    def _():
        mid_copy(1, 3, via_held, 1, 3).start()

    reach = FAR_WINDOW // FAR_DILATION
    apart, column = spacing(rows, rows, 0)
    valid = (apart >= 0) & (apart <= reach)
    distance = (apart * FAR_DILATION).astype(jnp.float32)
    lane = lax.broadcasted_iota(jnp.int32, (rows, HEAD_DIM), 1)
    packed = jnp.zeros((rows, HEAD_DIM), jnp.float32)
    for head in range(local_heads):
        at = head * HEAD_DIM
        attended, log_sum = attend(
            far_held[:, at : at + HEAD_DIM],
            far_held[:, width + at : width + at + HEAD_DIM],
            far_held[:, 2 * width + at : 2 * width + at + HEAD_DIM],
            slope_of(head, FAR_WINDOW), distance, valid,
        )
        back_send[:, at : at + HEAD_DIM] = attended.astype(jnp.bfloat16)
        rest = log_sum
        for term in range(3):
            piece = rest.astype(jnp.bfloat16).astype(jnp.float32)
            packed = jnp.where(lane == 3 * head + term, piece, packed)
            rest = rest - piece
    back_send[:, width:] = packed.astype(jnp.bfloat16)
    back_held[at_rows(me), :] = back_send[at_rows(me), :]
    each(lambda k: back_copy(k, True).start())

    @pl.when(me >= 1)
    def _():
        near_copy().wait_recv()
        mid_copy(1, 1, mid_own.at[0], 0, 1).wait_recv()
        mid_copy(1, 1, mid_own.at[1], 1, 1).wait_recv()

    @pl.when(relays)
    def _():
        mid_copy(0, 1, mid_held.at[1, 0], 0, 2).start()
        mid_copy(0, 1, mid_held.at[1, 1], 1, 2).start()

    apart, column = spacing(rows, NEAR_WINDOW + rows, NEAR_WINDOW)
    valid = (apart >= 0) & (apart <= NEAR_WINDOW) & (column + me * rows >= NEAR_WINDOW)
    distance = apart.astype(jnp.float32)
    near = []
    for head in range(local_heads):
        at = head * HEAD_DIM
        key = jnp.concatenate((near_held[:, at : at + HEAD_DIM], near_own[:, at : at + HEAD_DIM]), axis=0)
        at2 = width + at
        value = jnp.concatenate((near_held[:, at2 : at2 + HEAD_DIM], near_own[:, at2 : at2 + HEAD_DIM]), axis=0)
        near.append(attend(near_query[:, at : at + HEAD_DIM], key, value, slope_of(head, NEAR_WINDOW), distance, valid))

    @pl.when(me >= 2)
    def _():
        mid_copy(0, 2, mid_own.at[0], 0, 0).wait_recv()
        mid_copy(0, 2, mid_own.at[1], 1, 0).wait_recv()

    apart, column = spacing(rows, MIDDLE_WINDOW + rows, MIDDLE_WINDOW)
    valid = (apart >= 0) & (apart <= MIDDLE_WINDOW) & ((apart & (MIDDLE_DILATION - 1)) == 0)
    valid = valid & (column + me * rows >= MIDDLE_WINDOW)
    distance = apart.astype(jnp.float32)
    middle = []
    for head in range(local_heads):
        at = head * HEAD_DIM
        key = jnp.concatenate([x[:, at : at + HEAD_DIM] for x in (mid_held[0, 0], mid_held[1, 0], mid_own[0])], axis=0)
        value = jnp.concatenate([x[:, at : at + HEAD_DIM] for x in (mid_held[0, 1], mid_held[1, 1], mid_own[1])], axis=0)
        middle.append(attend(mid_query[:, at : at + HEAD_DIM], key, value, slope_of(head, MIDDLE_WINDOW), distance, valid))

    each(lambda k: back_copy(k, False).wait_recv())
    far = jnp.dot(swap, back_held[...], preferred_element_type=jnp.float32)
    parts = far[:, width:]
    totals = jnp.zeros((rows, HEAD_DIM), jnp.float32)
    for head in range(local_heads):
        at = head * HEAD_DIM
        far_log = jnp.sum(
            jnp.where((lane >= 3 * head) & (lane < 3 * head + 3), parts, 0.0), axis=-1, keepdims=True
        )
        near_log, middle_log = near[head][1], middle[head][1]
        highest = jnp.maximum(jnp.maximum(near_log, middle_log), far_log)
        total = highest + jnp.log(
            jnp.exp(near_log - highest) + jnp.exp(middle_log - highest) + jnp.exp(far_log - highest)
        )
        merged = near[head][0] * jnp.exp(near_log - total)
        merged = merged + middle[head][0] * jnp.exp(middle_log - total)
        merged = merged + far[:, at : at + HEAD_DIM] * jnp.exp(far_log - total)
        merged_own[:, at : at + HEAD_DIM] = merged.astype(jnp.bfloat16)
        totals = jnp.where(lane == head, total, totals)

    swap_merged = pltpu.make_async_remote_copy(
        src_ref=merged_own,
        dst_ref=merged_held,
        send_sem=merged_ssem,
        recv_sem=merged_rsem,
        device_id=(me, peer),
        device_id_type=MESH,
    )
    swap_merged.start()
    totals_ref[...] = totals
    both_ref[tp] = merged_own[...]
    swap_merged.wait_recv()
    both_ref[peer] = merged_held[...]

    swap_merged.wait_send()
    each(lambda k: far_copy(k, True).wait_send())
    each(lambda k: back_copy(k, True).wait_send())

    @pl.when(crosses)
    def _():
        via_copy().wait_send()

    @pl.when(sends_two)
    def _():
        mid_copy(0, 2, mid_own.at[0], 0, 0).wait_send()

    @pl.when(sends_two & jnp.logical_not(crosses))
    def _():
        mid_copy(0, 2, mid_own.at[1], 1, 0).wait_send()

    @pl.when(sends_one)
    def _():
        mid_copy(1, 1, mid_own.at[0], 0, 1).wait_send()
        near_copy().wait_send()

    @pl.when(own_value_one)
    def _():
        mid_copy(1, 1, mid_own.at[1], 1, 1).wait_send()

    @pl.when(forward_even)
    def _():
        mid_copy(0, 4, via_held, 1, 3).wait_send()

    @pl.when(forward_odd)
    def _():
        mid_copy(1, 3, via_held, 1, 3).wait_send()

    @pl.when(relays)
    def _():
        mid_copy(0, 1, mid_held.at[1, 0], 0, 2).wait_send()
        mid_copy(0, 1, mid_held.at[1, 1], 1, 2).wait_send()


def mix(both_ref, totals_ref, wo_ref, mixed_ref, log_ref):
    width = both_ref.shape[2]
    product = jnp.dot(both_ref[0], wo_ref[:width], preferred_element_type=jnp.float32)
    product = product + jnp.dot(both_ref[1], wo_ref[width:], preferred_element_type=jnp.float32)
    mixed_ref[...] = product.astype(jnp.bfloat16)
    log_ref[...] = jnp.transpose(totals_ref[...])[: log_ref.shape[0]]


def fused(n, n_tp, tokens, query_weight, key_weight, value_weight, out_weight):
    rows, depth = tokens.shape
    columns = query_weight.shape[1]
    local_heads = columns // (3 * HEAD_DIM)
    width = local_heads * HEAD_DIM
    dma = pltpu.SemaphoreType.DMA
    half = jnp.bfloat16
    both, totals = pl.pallas_call(
        functools.partial(kernel, n, n_tp, local_heads),
        out_shape=(
            jax.ShapeDtypeStruct((n_tp, rows, width), half),
            jax.ShapeDtypeStruct((rows, HEAD_DIM), jnp.float32),
        ),
        in_specs=[pl.BlockSpec(memory_space=pl.ANY)] * 4,
        out_specs=(pl.BlockSpec(memory_space=pltpu.VMEM), pl.BlockSpec(memory_space=pltpu.VMEM)),
        scratch_shapes=[
            pltpu.VMEM((rows, depth), half),
            pltpu.VMEM((3, depth, columns), half),
            pltpu.VMEM((rows, columns), half),
            pltpu.VMEM((rows, columns), half),
            pltpu.VMEM((rows, width + HEAD_DIM), half),
            pltpu.VMEM((rows, width + HEAD_DIM), half),
            pltpu.VMEM((rows, width), half),
            pltpu.VMEM((2, rows, width), half),
            pltpu.VMEM((2, 2, rows, width), half),
            pltpu.VMEM((rows, width), half),
            pltpu.VMEM((rows, width), half),
            pltpu.VMEM((rows, 2 * width), half),
            pltpu.VMEM((NEAR_WINDOW, 2 * width), half),
            pltpu.VMEM((rows, width), half),
            pltpu.VMEM((rows, width), half),
            dma((1 + 9 * local_heads,)),
            dma((n,)), dma((n,)), dma((n,)), dma((n,)),
            dma((4, 2)), dma((2, 2)), dma(()), dma(()), dma(()), dma(()), dma(()), dma(()),
        ],
        compiler_params=pltpu.CompilerParams(
            collective_id=0, has_side_effects=True, vmem_limit_bytes=63900 * 1024
        ),
    )(tokens, query_weight, key_weight, value_weight)
    whole = pl.BlockSpec(memory_space=pltpu.VMEM)
    return pl.pallas_call(
        mix,
        out_shape=(
            jax.ShapeDtypeStruct((rows, out_weight.shape[1]), half),
            jax.ShapeDtypeStruct((local_heads, rows), jnp.float32),
        ),
        in_specs=[whole] * 3,
        out_specs=(whole, whole),
        compiler_params=pltpu.CompilerParams(vmem_limit_bytes=16000 * 1024),
    )(both, totals, out_weight)


def solution(mesh):
    n, n_tp = mesh.shape["sp"], mesh.shape["tp"]
    if n == FAR_DILATION and n_tp == 2:
        body = functools.partial(fused, n, n_tp)
    else:
        body = local
    return jax.shard_map(
        body,
        mesh=mesh,
        in_specs=(P("sp", None), P(None, "tp"), P(None, "tp"), P(None, "tp"), P(None, "tp")),
        out_specs=(P("sp", "tp"), P("tp", "sp")),
        check_vma=False,
    )
```

```python
import functools
import jax
import jax.numpy as jnp
from jax import lax
from jax.experimental import pallas as pl
from jax.experimental.pallas import tpu as pltpu
from jax.sharding import PartitionSpec as P

HEADS = 4
HEAD_DIM = 128
NEAR_WINDOW = 128
MIDDLE_WINDOW = 512
MIDDLE_DILATION = 4
FAR_WINDOW = 2048
FAR_DILATION = 16


def from_behind(block, axis, distance):
    devices = range(lax.axis_size(axis))
    route = [(i - distance, i) for i in devices if i - distance in devices]
    return lax.ppermute(block, axis, route)


def window_table():
    return ((NEAR_WINDOW, 1), (MIDDLE_WINDOW, MIDDLE_DILATION), (FAR_WINDOW, FAR_DILATION))


def tail_counts(row_count, distance, held_rows):
    counts = []
    for entry, available in zip(window_table(), held_rows):
        counts.append(max(0, min(available, entry[0] - (distance - 1) * row_count)))
    return counts


def pack_tails(sources, counts):
    selected = [
        source[:, source.shape[1] - amount :]
        for source, amount in zip(sources, counts)
        if amount > 0
    ]
    return jnp.concatenate(selected, axis=1)


def unpack_rows(packed, counts):
    result = []
    cursor = 0
    for amount in counts:
        result.append(packed[:, cursor : cursor + amount])
        cursor = cursor + amount
    return result


def attend_group(group_queries, buffer, window, dilation, first_key, slopes_here):
    row_count = group_queries.shape[0]
    head_count = group_queries.shape[1]
    head_size = group_queries.shape[2]
    query_split = group_queries.reshape(row_count // dilation, dilation, head_count, head_size)
    key_split = buffer[0].reshape(-1, dilation, head_count, head_size)
    value_split = buffer[1].reshape(-1, dilation, head_count, head_size)
    scores = jnp.einsum(
        "mrhe,nrhe->rhmn", query_split, key_split, preferred_element_type=jnp.float32
    ) * head_size ** (-0.5)
    grid_shape = (row_count // dilation, key_split.shape[0])
    query_slot = lax.broadcasted_iota(jnp.int32, grid_shape, 0)
    key_slot = lax.broadcasted_iota(jnp.int32, grid_shape, 1)
    spacing = query_slot + window // dilation - key_slot
    residue = lax.broadcasted_iota(jnp.int32, (dilation, 1, 1), 0)
    key_place = first_key + residue + dilation * key_slot[None]
    valid = (spacing[None] >= 0) & (spacing[None] <= window // dilation) & (key_place >= 0)
    scores = (
        scores
        - slopes_here[None, :, None, None] * (dilation * spacing).astype(jnp.float32)[None, None]
    )
    masked = jnp.where(valid[:, None], scores, -jnp.inf)
    highest = jnp.max(masked, axis=-1, keepdims=True)
    log_sum = highest + jnp.log(jnp.sum(jnp.exp(masked - highest), axis=-1, keepdims=True))
    probs = jnp.exp(masked - log_sum).astype(jnp.bfloat16)
    attended = jnp.einsum("rhmn,nrhe->mrhe", probs, value_split, preferred_element_type=jnp.float32)
    attended = attended.reshape(row_count, head_count, head_size)
    log_rows = jnp.transpose(log_sum[..., 0], (1, 2, 0)).reshape(head_count, row_count)
    return (attended, log_rows)


def local(tokens, query_weight, key_weight, value_weight, out_weight):
    rows_here = tokens.shape[0]
    local_heads = query_weight.shape[1] // (3 * HEAD_DIM)

    def project(weight_matrix):
        product = jnp.dot(tokens, weight_matrix, preferred_element_type=jnp.float32)
        return product.astype(jnp.bfloat16).reshape(rows_here, local_heads, 3, HEAD_DIM)

    queries = project(query_weight)
    keys_all = project(key_weight)
    values_all = project(value_weight)
    table = window_table()
    own = [jnp.stack((keys_all[:, :, index], values_all[:, :, index])) for index in range(3)]
    held = list(own)
    span_now = 1
    while span_now * rows_here < FAR_WINDOW + rows_here:
        counts = tail_counts(rows_here, span_now, [item.shape[1] for item in held])
        packed = pack_tails(held, counts)
        arrived = from_behind(packed, "sp", span_now)
        pieces_in = unpack_rows(arrived, counts)
        for index in range(3):
            if counts[index] > 0:
                joined = jnp.concatenate((pieces_in[index], held[index]), axis=1)
                held[index] = joined
        span_now = span_now * 2
    priors = [held[index][:, : table[index][0]] for index in range(3)]
    position_start = lax.axis_index("sp") * rows_here
    head_ids = (
        lax.axis_index("tp") * local_heads + jnp.arange(local_heads, dtype=jnp.int32)
    ).astype(jnp.float32)
    outputs = []
    logs = []
    for index, (window, dilation) in enumerate(table):
        buffer = jnp.concatenate((priors[index], own[index]), axis=1)
        slopes_here = 2.0 ** (3.0 - 8.0 * (head_ids + 1.0) / HEADS) / window
        attended, log_rows = attend_group(
            queries[:, :, index], buffer, window, dilation, position_start - window, slopes_here
        )
        outputs.append(attended)
        logs.append(log_rows)
    stacked_logs = jnp.stack(logs)
    highest = jnp.max(stacked_logs, axis=0)
    total_log = highest + jnp.log(jnp.sum(jnp.exp(stacked_logs - highest), axis=0))
    mixing = jnp.exp(stacked_logs - total_log)
    merged = outputs[0] * jnp.transpose(mixing[0])[:, :, None]
    merged = merged + outputs[1] * jnp.transpose(mixing[1])[:, :, None]
    merged = merged + outputs[2] * jnp.transpose(mixing[2])[:, :, None]
    merged = merged.astype(jnp.bfloat16).reshape(rows_here, local_heads * HEAD_DIM)
    mixed = jnp.dot(
        lax.all_gather(merged, "tp", axis=1, tiled=True),
        out_weight,
        preferred_element_type=jnp.float32,
    ).astype(jnp.bfloat16)
    return (mixed, total_log)


MESH = pl.DeviceIdType.MESH
MASKED = -1e30


def attend(query, key, value, slope, distance, valid):
    scores = lax.dot_general(
        query, key, (((1,), (1,)), ((), ())), preferred_element_type=jnp.float32
    ) * HEAD_DIM ** (-0.5)
    scores = jnp.where(valid, scores - slope * distance, MASKED)
    highest = jnp.max(scores, axis=-1, keepdims=True)
    weights = jnp.exp(scores - highest)
    total = jnp.sum(weights, axis=-1, keepdims=True)
    probs = (weights * (1.0 / total)).astype(jnp.bfloat16)
    attended = jnp.dot(probs, value, preferred_element_type=jnp.float32)
    return attended, highest + jnp.log(total)


def swap_matrix(rows, width):
    shift = width.bit_length() - 1
    row = lax.broadcasted_iota(jnp.int32, (rows, rows), 0)
    column = lax.broadcasted_iota(jnp.int32, (rows, rows), 1)
    source = ((row & (width - 1)) << shift) + (row >> shift)
    return jnp.where(column == source, 1.0, 0.0).astype(jnp.bfloat16)


def kernel(
    n, n_tp, local_heads,
    tok_hbm, wq_hbm, wk_hbm, wv_hbm,
    both_ref, totals_ref,
    tok, weight, far_send, far_held, back_send, back_held,
    mid_query, mid_own, mid_held, via_held, near_query, near_own, near_held,
    merged_own, merged_held,
    load_sem, far_ssem, far_rsem, back_ssem, back_rsem,
    mid_ssem, mid_rsem, via_ssem, via_rsem, near_ssem, near_rsem, merged_ssem, merged_rsem,
):
    me = lax.axis_index("sp")
    tp = lax.axis_index("tp")
    rows = tok.shape[0]
    width = local_heads * HEAD_DIM
    chunk = rows // n
    peer = 1 - tp

    loads = {}
    tok_load = pltpu.make_async_copy(tok_hbm, tok, load_sem.at[0])
    tok_load.start()
    count = 1
    for group in (2, 1, 0):
        loads[group] = []
        for part, source in enumerate((wq_hbm, wk_hbm, wv_hbm)):
            for head in range(local_heads):
                copy = pltpu.make_async_copy(
                    source.at[:, pl.ds((head * 3 + group) * HEAD_DIM, HEAD_DIM)],
                    weight.at[group, :, pl.ds((part * local_heads + head) * HEAD_DIM, HEAD_DIM)],
                    load_sem.at[count],
                )
                copy.start()
                loads[group].append(copy)
                count += 1

    barrier = pltpu.get_barrier_semaphore()

    def greet(k, carry):
        pl.semaphore_signal(barrier, inc=1, device_id=(lax.rem(me + k, n), tp), device_id_type=MESH)
        return carry

    lax.fori_loop(1, n, greet, 0)
    pl.semaphore_signal(barrier, inc=1, device_id=(me, peer), device_id_type=MESH)

    @pl.when(me < 2)
    def _():
        mid_held[0] = jnp.zeros((2, rows, width), jnp.bfloat16)

    @pl.when(me < 1)
    def _():
        mid_held[1] = jnp.zeros((2, rows, width), jnp.bfloat16)
        near_held[...] = jnp.zeros((NEAR_WINDOW, 2 * width), jnp.bfloat16)

    def project(group, first, extent):
        return jnp.dot(
            tok[...], weight[group, :, first : first + extent], preferred_element_type=jnp.float32
        ).astype(jnp.bfloat16)

    def at_rows(index):
        return pl.ds(pl.multiple_of(index * chunk, chunk), chunk)

    swap = swap_matrix(rows, n)
    tok_load.wait()
    for part in range(3):
        for copy in loads[2][part * local_heads : (part + 1) * local_heads]:
            copy.wait()
        block = project(2, part * width, width)
        far_send[:, part * width : (part + 1) * width] = jnp.dot(
            swap, block, preferred_element_type=jnp.float32
        ).astype(jnp.bfloat16)
    far_held[at_rows(me), :] = far_send[at_rows(me), :]

    def exchange(source, target, ssem, rsem, k, outgoing):
        to = lax.rem(me + k, n)
        come = lax.rem(me + n - k, n)
        return pltpu.make_async_remote_copy(
            src_ref=source.at[at_rows(to)],
            dst_ref=target.at[at_rows(me if outgoing else come)],
            send_sem=ssem.at[k],
            recv_sem=rsem.at[k],
            device_id=(to, tp),
            device_id_type=MESH,
        )

    def far_copy(k, outgoing):
        return exchange(far_send, far_held, far_ssem, far_rsem, k, outgoing)

    def back_copy(k, outgoing):
        return exchange(back_send, back_held, back_ssem, back_rsem, k, outgoing)

    def each(action):
        def step(k, carry):
            action(k)
            return carry

        lax.fori_loop(1, n, step, 0)

    pl.semaphore_wait(barrier, n)
    each(lambda k: far_copy(k, True).start())

    for copy in loads[1]:
        copy.wait()
    mid_own[0] = project(1, width, width)
    mid_own[1] = project(1, 2 * width, width)

    def mid_copy(slot, hop, source, part, sem):
        return pltpu.make_async_remote_copy(
            src_ref=source,
            dst_ref=mid_held.at[slot, part],
            send_sem=mid_ssem.at[sem, part],
            recv_sem=mid_rsem.at[slot, part],
            device_id=(lax.rem(me + hop + n, n), tp),
            device_id_type=MESH,
        )

    def via_copy():
        return pltpu.make_async_remote_copy(
            src_ref=mid_own.at[1],
            dst_ref=via_held,
            send_sem=via_ssem,
            recv_sem=via_rsem,
            device_id=(lax.rem(me + -2 + n, n), tp),
            device_id_type=MESH,
        )

    def near_copy():
        return pltpu.make_async_remote_copy(
            src_ref=near_own.at[pl.ds(rows - NEAR_WINDOW, NEAR_WINDOW)],
            dst_ref=near_held,
            send_sem=near_ssem,
            recv_sem=near_rsem,
            device_id=(lax.rem(me + 1, n), tp),
            device_id_type=MESH,
        )

    even = lax.rem(me, 2) == 0
    sends_one = me + 1 < n
    sends_two = even & (me + 2 < n)
    relays = even & (me >= 1)

    crosses = (lax.rem(me, 4) >= 2) & sends_one & (me + 4 - lax.rem(me, 4) < n)
    forwards = (lax.rem(me, 4) < 2) & (me + 4 - lax.rem(me, 4) < n)
    forward_even = forwards & even
    forward_odd = forwards & jnp.logical_not(even)

    @pl.when(crosses)
    def _():
        via_copy().start()

    @pl.when(sends_two)
    def _():
        mid_copy(0, 2, mid_own.at[0], 0, 0).start()

    @pl.when(sends_one)
    def _():
        mid_copy(1, 1, mid_own.at[0], 0, 1).start()

    @pl.when(sends_two & jnp.logical_not(crosses))
    def _():
        mid_copy(0, 2, mid_own.at[1], 1, 0).start()

    own_value_one = sends_one & jnp.logical_not(crosses & jnp.logical_not(even))

    @pl.when(own_value_one)
    def _():
        mid_copy(1, 1, mid_own.at[1], 1, 1).start()

    for copy in loads[0]:
        copy.wait()
    near_own[:, :width] = project(0, width, width)
    near_own[:, width:] = project(0, 2 * width, width)

    @pl.when(sends_one)
    def _():
        near_copy().start()

    mid_query[...] = project(1, 0, width)
    near_query[...] = project(0, 0, width)

    def slope_of(head, window):
        number = tp * local_heads + head
        slope = jnp.float32(0.0)
        for index in range(HEADS):
            value = 2.0 ** (3.0 - 8.0 * (index + 1.0) / HEADS) / window
            slope = jnp.where(number == index, jnp.float32(value), slope)
        return slope

    def spacing(row_count, key_count, offset):
        row = lax.broadcasted_iota(jnp.int32, (row_count, key_count), 0)
        column = lax.broadcasted_iota(jnp.int32, (row_count, key_count), 1)
        return row + offset - column, column

    each(lambda k: far_copy(k, False).wait_recv())

    @pl.when(forwards)
    def _():
        via_copy().wait_recv()

    @pl.when(forward_even)
    def _():
        mid_copy(0, 4, via_held, 1, 3).start()

    @pl.when(forward_odd)
    def _():
        mid_copy(1, 3, via_held, 1, 3).start()

    reach = FAR_WINDOW // FAR_DILATION
    apart, column = spacing(rows, rows, 0)
    valid = (apart >= 0) & (apart <= reach)
    distance = (apart * FAR_DILATION).astype(jnp.float32)
    lane = lax.broadcasted_iota(jnp.int32, (rows, HEAD_DIM), 1)
    packed = jnp.zeros((rows, HEAD_DIM), jnp.float32)
    for head in range(local_heads):
        at = head * HEAD_DIM
        attended, log_sum = attend(
            far_held[:, at : at + HEAD_DIM],
            far_held[:, width + at : width + at + HEAD_DIM],
            far_held[:, 2 * width + at : 2 * width + at + HEAD_DIM],
            slope_of(head, FAR_WINDOW), distance, valid,
        )
        back_send[:, at : at + HEAD_DIM] = attended.astype(jnp.bfloat16)
        rest = log_sum
        for term in range(3):
            piece = rest.astype(jnp.bfloat16).astype(jnp.float32)
            packed = jnp.where(lane == 3 * head + term, piece, packed)
            rest = rest - piece
    back_send[:, width:] = packed.astype(jnp.bfloat16)
    back_held[at_rows(me), :] = back_send[at_rows(me), :]
    each(lambda k: back_copy(k, True).start())

    @pl.when(me >= 1)
    def _():
        near_copy().wait_recv()
        mid_copy(1, 1, mid_own.at[0], 0, 1).wait_recv()
        mid_copy(1, 1, mid_own.at[1], 1, 1).wait_recv()

    @pl.when(relays)
    def _():
        mid_copy(0, 1, mid_held.at[1, 0], 0, 2).start()
        mid_copy(0, 1, mid_held.at[1, 1], 1, 2).start()

    apart, column = spacing(rows, NEAR_WINDOW + rows, NEAR_WINDOW)
    valid = (apart >= 0) & (apart <= NEAR_WINDOW) & (column + me * rows >= NEAR_WINDOW)
    distance = apart.astype(jnp.float32)
    near = []
    for head in range(local_heads):
        at = head * HEAD_DIM
        key = jnp.concatenate((near_held[:, at : at + HEAD_DIM], near_own[:, at : at + HEAD_DIM]), axis=0)
        at2 = width + at
        value = jnp.concatenate((near_held[:, at2 : at2 + HEAD_DIM], near_own[:, at2 : at2 + HEAD_DIM]), axis=0)
        near.append(attend(near_query[:, at : at + HEAD_DIM], key, value, slope_of(head, NEAR_WINDOW), distance, valid))

    @pl.when(me >= 2)
    def _():
        mid_copy(0, 2, mid_own.at[0], 0, 0).wait_recv()
        mid_copy(0, 2, mid_own.at[1], 1, 0).wait_recv()

    apart, column = spacing(rows, MIDDLE_WINDOW + rows, MIDDLE_WINDOW)
    valid = (apart >= 0) & (apart <= MIDDLE_WINDOW) & ((apart & (MIDDLE_DILATION - 1)) == 0)
    valid = valid & (column + me * rows >= MIDDLE_WINDOW)
    distance = apart.astype(jnp.float32)
    middle = []
    for head in range(local_heads):
        at = head * HEAD_DIM
        key = jnp.concatenate([x[:, at : at + HEAD_DIM] for x in (mid_held[0, 0], mid_held[1, 0], mid_own[0])], axis=0)
        value = jnp.concatenate([x[:, at : at + HEAD_DIM] for x in (mid_held[0, 1], mid_held[1, 1], mid_own[1])], axis=0)
        middle.append(attend(mid_query[:, at : at + HEAD_DIM], key, value, slope_of(head, MIDDLE_WINDOW), distance, valid))

    each(lambda k: back_copy(k, False).wait_recv())
    far = jnp.dot(swap, back_held[...], preferred_element_type=jnp.float32)
    parts = far[:, width:]
    totals = jnp.zeros((rows, HEAD_DIM), jnp.float32)
    for head in range(local_heads):
        at = head * HEAD_DIM
        far_log = jnp.sum(
            jnp.where((lane >= 3 * head) & (lane < 3 * head + 3), parts, 0.0), axis=-1, keepdims=True
        )
        near_log, middle_log = near[head][1], middle[head][1]
        highest = jnp.maximum(jnp.maximum(near_log, middle_log), far_log)
        total = highest + jnp.log(
            jnp.exp(near_log - highest) + jnp.exp(middle_log - highest) + jnp.exp(far_log - highest)
        )
        merged = near[head][0] * jnp.exp(near_log - total)
        merged = merged + middle[head][0] * jnp.exp(middle_log - total)
        merged = merged + far[:, at : at + HEAD_DIM] * jnp.exp(far_log - total)
        merged_own[:, at : at + HEAD_DIM] = merged.astype(jnp.bfloat16)
        totals = jnp.where(lane == head, total, totals)

    swap_merged = pltpu.make_async_remote_copy(
        src_ref=merged_own,
        dst_ref=merged_held,
        send_sem=merged_ssem,
        recv_sem=merged_rsem,
        device_id=(me, peer),
        device_id_type=MESH,
    )
    swap_merged.start()
    totals_ref[...] = totals
    both_ref[tp] = merged_own[...]
    swap_merged.wait_recv()
    both_ref[peer] = merged_held[...]

    swap_merged.wait_send()
    each(lambda k: far_copy(k, True).wait_send())
    each(lambda k: back_copy(k, True).wait_send())

    @pl.when(crosses)
    def _():
        via_copy().wait_send()

    @pl.when(sends_two)
    def _():
        mid_copy(0, 2, mid_own.at[0], 0, 0).wait_send()

    @pl.when(sends_two & jnp.logical_not(crosses))
    def _():
        mid_copy(0, 2, mid_own.at[1], 1, 0).wait_send()

    @pl.when(sends_one)
    def _():
        mid_copy(1, 1, mid_own.at[0], 0, 1).wait_send()
        near_copy().wait_send()

    @pl.when(own_value_one)
    def _():
        mid_copy(1, 1, mid_own.at[1], 1, 1).wait_send()

    @pl.when(forward_even)
    def _():
        mid_copy(0, 4, via_held, 1, 3).wait_send()

    @pl.when(forward_odd)
    def _():
        mid_copy(1, 3, via_held, 1, 3).wait_send()

    @pl.when(relays)
    def _():
        mid_copy(0, 1, mid_held.at[1, 0], 0, 2).wait_send()
        mid_copy(0, 1, mid_held.at[1, 1], 1, 2).wait_send()


def mix(both_ref, totals_ref, wo_ref, mixed_ref, log_ref):
    width = both_ref.shape[2]
    product = jnp.dot(both_ref[0], wo_ref[:width], preferred_element_type=jnp.float32)
    product = product + jnp.dot(both_ref[1], wo_ref[width:], preferred_element_type=jnp.float32)
    mixed_ref[...] = product.astype(jnp.bfloat16)
    log_ref[...] = jnp.transpose(totals_ref[...])[: log_ref.shape[0]]


def fused(n, n_tp, tokens, query_weight, key_weight, value_weight, out_weight):
    rows, depth = tokens.shape
    columns = query_weight.shape[1]
    local_heads = columns // (3 * HEAD_DIM)
    width = local_heads * HEAD_DIM
    dma = pltpu.SemaphoreType.DMA
    half = jnp.bfloat16
    both, totals = pl.pallas_call(
        functools.partial(kernel, n, n_tp, local_heads),
        out_shape=(
            jax.ShapeDtypeStruct((n_tp, rows, width), half),
            jax.ShapeDtypeStruct((rows, HEAD_DIM), jnp.float32),
        ),
        in_specs=[pl.BlockSpec(memory_space=pl.ANY)] * 4,
        out_specs=(pl.BlockSpec(memory_space=pltpu.VMEM), pl.BlockSpec(memory_space=pltpu.VMEM)),
        scratch_shapes=[
            pltpu.VMEM((rows, depth), half),
            pltpu.VMEM((3, depth, columns), half),
            pltpu.VMEM((rows, columns), half),
            pltpu.VMEM((rows, columns), half),
            pltpu.VMEM((rows, width + HEAD_DIM), half),
            pltpu.VMEM((rows, width + HEAD_DIM), half),
            pltpu.VMEM((rows, width), half),
            pltpu.VMEM((2, rows, width), half),
            pltpu.VMEM((2, 2, rows, width), half),
            pltpu.VMEM((rows, width), half),
            pltpu.VMEM((rows, width), half),
            pltpu.VMEM((rows, 2 * width), half),
            pltpu.VMEM((NEAR_WINDOW, 2 * width), half),
            pltpu.VMEM((rows, width), half),
            pltpu.VMEM((rows, width), half),
            dma((1 + 9 * local_heads,)),
            dma((n,)), dma((n,)), dma((n,)), dma((n,)),
            dma((4, 2)), dma((2, 2)), dma(()), dma(()), dma(()), dma(()), dma(()), dma(()),
        ],
        compiler_params=pltpu.CompilerParams(
            collective_id=0, has_side_effects=True, vmem_limit_bytes=54000 * 1024
        ),
    )(tokens, query_weight, key_weight, value_weight)
    whole = pl.BlockSpec(memory_space=pltpu.VMEM)
    return pl.pallas_call(
        mix,
        out_shape=(
            jax.ShapeDtypeStruct((rows, out_weight.shape[1]), half),
            jax.ShapeDtypeStruct((local_heads, rows), jnp.float32),
        ),
        in_specs=[whole] * 3,
        out_specs=(whole, whole),
        compiler_params=pltpu.CompilerParams(vmem_limit_bytes=16000 * 1024),
    )(both, totals, out_weight)


def solution(mesh):
    n, n_tp = mesh.shape["sp"], mesh.shape["tp"]
    if n == FAR_DILATION and n_tp == 2:
        body = functools.partial(fused, n, n_tp)
    else:
        body = local
    return jax.shard_map(
        body,
        mesh=mesh,
        in_specs=(P("sp", None), P(None, "tp"), P(None, "tp"), P(None, "tp"), P(None, "tp")),
        out_specs=(P("sp", "tp"), P("tp", "sp")),
        check_vma=False,
    )
```
